32 devices in a mesh: sp: 8 (over z, y), tp: 4 (over x, core).
Axes of the slice: x: 2, y: 2, z: 4, core: 2. Of those that a mesh axis runs over, the one named last changes fastest.
Arguments:
- query_first: bfloat16 [6144, 8, 128], P('sp', 'tp'), may hold values from -5.375 to 5.375
- key_first: bfloat16 [6144, 8, 128], P('sp', 'tp'), may hold values from -5.375 to 5.375
- value_first: bfloat16 [6144, 8, 128], P('sp', 'tp'), may hold values from -6 to 6
- query_second: bfloat16 [6144, 8, 256], P('sp', 'tp'), may hold values from -5.375 to 5.375
- key_second: bfloat16 [6144, 8, 256], P('sp', 'tp'), may hold values from -5.375 to 5.375
- value_second: bfloat16 [6144, 8, 128], P('sp', 'tp'), may hold values from -6 to 6
- mix_lambda: float32 [2, 8], P(None, 'tp'), may hold values from 0.3 to 0.8
- head_gain: float32 [2, 8, 128], P(None, 'tp'), may hold values from 0.1 to 1.9
- out_weight: bfloat16 [2, 8, 128, 2048], P(None, 'tp'), may hold values from -0.125 to 0.125
- residual: bfloat16 [6144, 2048], P(('sp', 'tp')), may hold values from -6 to 6
- norm_gain: float32 [2, 2048], replicated, may hold values from 0.1 to 1.9
- up_weight: bfloat16 [2048, 8192], P('sp', 'tp'), may hold values from -0.125 to 0.125
- down_weight: bfloat16 [8192, 2048], P('tp', 'sp'), may hold values from -0.0625 to 0.0625
Outputs:
- mixed: bfloat16 [6144, 2048], P(('sp', 'tp'))
The draws below stay inside these ranges and needn't reach their ends.
All inputs are finite; a program needn't handle non-finite values.
Results may differ from the reference program's by a relative error of at most 0.02.
Values may be sent and summed in bfloat16 or wider, within the bound.
A program may use at most 128 MiB of HBM per device.

```python
import math
import jax
import jax.numpy as jnp
from jax import lax

D = 2048
FF = 8192
HEADS = 8
KA = 64
KB = 128
VD = 128
TOK_DEV = 768
TOKENS = 6144
N_SP = 8


def drawn_pair(key, group_tag, key_size):
    seeded = jax.random.fold_in(key, group_tag)
    seed_query, seed_keys = jax.random.split(seeded, 2)
    array_shape = (TOKENS, HEADS, 2 * key_size)
    queries = 1.3 * jax.random.truncated_normal(seed_query, -3.4, 3.4, array_shape, jnp.float32)
    key_rows = 1.3 * jax.random.truncated_normal(seed_keys, -3.4, 3.4, array_shape, jnp.float32)
    return (queries, key_rows)


def draw_query_first(key, part):
    return drawn_pair(key, 11, KA)[0].astype(jnp.bfloat16)


def draw_key_first(key, part):
    return drawn_pair(key, 11, KA)[1].astype(jnp.bfloat16)


def draw_query_second(key, part):
    return drawn_pair(key, 23, KB)[0].astype(jnp.bfloat16)


def draw_key_second(key, part):
    return drawn_pair(key, 23, KB)[1].astype(jnp.bfloat16)


def shard_levels(own_key, dims, cuts, smallest, high):
    def one(position, blocks):
        heights = jax.random.uniform(jax.random.fold_in(jax.random.fold_in(own_key, 6), position), (blocks,), jnp.float32, smallest / len(cuts), high / len(cuts))
        return jnp.repeat(jnp.exp(heights), dims[position] // blocks).reshape((-1,) + (1,) * (len(dims) - position - 1))

    loudness = one(*cuts[0])
    for cut in cuts[1:]:
        loudness = loudness * one(*cut)
    return loudness


def scatter_about(key, shape, deviation, limit, cuts=(), kind=jnp.bfloat16):
    drawn = deviation * jax.random.normal(key, shape, jnp.float32)
    if cuts:
        drawn = drawn * shard_levels(key, shape, cuts, -0.22, 0.18)
    return jnp.clip(drawn, -limit, limit).astype(kind)


def setup_inputs(seed: int = 0) -> dict:
    seeds = jax.random.split(jax.random.key(seed), 14)
    return {
        "query_first": draw_query_first(jax.random.fold_in(seeds[13], 71), 0),
        "key_first": draw_key_first(jax.random.fold_in(seeds[13], 71), 0),
        "value_first": scatter_about(seeds[2], (TOKENS, HEADS, VD), 1.0, 6.0, ((0, 8), (1, 4))),
        "query_second": draw_query_second(jax.random.fold_in(seeds[13], 71), 0),
        "key_second": draw_key_second(jax.random.fold_in(seeds[13], 71), 0),
        "value_second": scatter_about(seeds[5], (TOKENS, HEADS, VD), 1.0, 6.0, ((0, 8), (1, 4))),
        "mix_lambda": jnp.clip(0.3 + 0.5 * jax.random.uniform(seeds[6], (2, HEADS), jnp.float32) ** shard_levels(seeds[6], (2, HEADS), ((1, 4),), -0.2, 0.2), 0.3, 0.8),
        "head_gain": jnp.clip(1.0 + 0.18 * jax.random.normal(seeds[7], (2, HEADS, VD), jnp.float32), 0.1, 1.9),
        "out_weight": scatter_about(seeds[8], (2, HEADS, VD, D), D ** -0.5, 0.125, ((1, 4),)),
        "residual": scatter_about(seeds[9], (TOKENS, D), 1.0, 6.0, ((0, 32),)),
        "norm_gain": jnp.clip(1.0 + 0.18 * jax.random.normal(seeds[10], (2, D), jnp.float32), 0.1, 1.9),
        "up_weight": scatter_about(seeds[11], (D, FF), D ** -0.5, 0.125, ((0, 8), (1, 4))),
        "down_weight": scatter_about(seeds[12], (FF, D), FF ** -0.5, 0.0625, ((0, 4), (1, 8))),
    }


EPSILON = 1e-05

def layer_norm(activations, scales):
    average = lax.optimization_barrier(jnp.mean(activations, axis=-1, keepdims=True))
    centred = activations - average
    spread = lax.optimization_barrier(jnp.mean(centred * centred, axis=-1, keepdims=True))
    return centred * lax.rsqrt(spread + EPSILON) * scales

def group_attention(queries_in, keys_in, values_in, lambdas, gains, key_size):
    score_scale = 1.0 / math.sqrt(key_size)
    queries = queries_in.astype(jnp.float32).reshape(TOKENS, HEADS, 2, key_size)
    key_rows = keys_in.astype(jnp.float32).reshape(TOKENS, HEADS, 2, key_size)
    value_rows = values_in.astype(jnp.float32)
    query_blocks = queries.reshape(N_SP, TOK_DEV, HEADS, 2, key_size)

    def one_block(query_block):
        scores = jnp.einsum('qhck,phck->hcqp', query_block, key_rows) * score_scale
        peak = lax.optimization_barrier(jnp.max(scores, axis=-1, keepdims=True))
        exponent = jnp.exp(scores - peak)
        denominator = lax.optimization_barrier(jnp.sum(exponent, axis=-1))
        rounded = lax.optimization_barrier(exponent.astype(jnp.bfloat16)).astype(jnp.float32)
        numerator = jnp.einsum('hcqp,phv->hcqv', rounded, value_rows)
        attended = numerator[:, 0] / denominator[:, 0, :, None] - lambdas[:, None, None] * numerator[:, 1] / denominator[:, 1, :, None]
        mean_square = lax.optimization_barrier(jnp.mean(attended * attended, axis=-1, keepdims=True))
        return (attended * lax.rsqrt(mean_square + EPSILON) * gains[:, None, :]).astype(jnp.bfloat16)
    blocks_out = lax.map(one_block, query_blocks)
    return blocks_out.transpose(1, 0, 2, 3).reshape(HEADS, TOKENS, VD)

def reference(query_first, key_first, value_first, query_second, key_second, value_second, mix_lambda, head_gain, out_weight, residual, norm_gain, up_weight, down_weight):
    heads_first = group_attention(query_first, key_first, value_first, mix_lambda[0], head_gain[0], KA)
    heads_second = group_attention(query_second, key_second, value_second, mix_lambda[1], head_gain[1], KB)
    stacked = jnp.stack([heads_first, heads_second]).astype(jnp.float32)
    projected = jnp.einsum('ghtv,ghvd->td', stacked, out_weight.astype(jnp.float32)) + residual.astype(jnp.float32)
    normed = layer_norm(projected, norm_gain[0])
    expanded = jnp.dot(normed.astype(jnp.bfloat16), up_weight, preferred_element_type=jnp.float32)
    hidden = jnp.square(jnp.maximum(expanded, 0.0)).astype(jnp.bfloat16)
    mixed_sum = jnp.dot(hidden, down_weight, preferred_element_type=jnp.float32)
    return layer_norm(normed + mixed_sum, norm_gain[1]).astype(jnp.bfloat16)
```

```python
import functools
import math

import jax
import jax.numpy as jnp
from jax import lax
from jax.experimental import pallas as pl
from jax.experimental.pallas import tpu as pltpu
from jax.sharding import PartitionSpec as P

EPSILON = 1e-05


def layer_norm(activations, scales):
    average = jnp.mean(activations, axis=-1, keepdims=True)
    centred = activations - average
    spread = jnp.mean(centred * centred, axis=-1, keepdims=True)
    return centred * lax.rsqrt(spread + EPSILON) * scales


def largest_divisor(length, choices):
    for choice in choices:
        if length % choice == 0:
            return choice
    return length


def attention_kernel(lambda_ref, query_ref, key_ref, value_ref, gain_ref, out_ref, wide_ref, *, score_scale, key_block):
    queries, width = query_ref.shape
    size = width // 2
    tokens, value_size = value_ref.shape

    @pl.when(pl.program_id(1) == 0)
    def widen():
        wide_ref[:, :value_size] = value_ref[...]
        wide_ref[:, value_size:] = jnp.ones((tokens, value_size), jnp.bfloat16)

    factor = score_scale * math.log2(math.e)
    maxima, sums = [None, None], [None, None]
    for start in range(0, tokens, key_block):
        for c in range(2):
            scores = lax.dot_general(
                query_ref[:, c * size : (c + 1) * size],
                key_ref[start : start + key_block, c * size : (c + 1) * size],
                (((1,), (1,)), ((), ())),
                preferred_element_type=jnp.float32,
            )
            newest = jnp.max(scores, axis=-1, keepdims=True)
            if start:
                newest = jnp.maximum(maxima[c], newest)
            weights = jnp.exp2((scores - newest) * factor).astype(jnp.bfloat16)
            summed = jnp.dot(
                weights, wide_ref[start : start + key_block, :], preferred_element_type=jnp.float32
            )
            if start:
                summed = summed + sums[c] * jnp.exp2((maxima[c] - newest) * factor)
            maxima[c], sums[c] = newest, summed
    one, two = (member[:, :value_size] / member[:, value_size:] for member in sums)
    attended = one - lambda_ref[pl.program_id(0)] * two
    mean_square = jnp.mean(attended * attended, axis=-1, keepdims=True)
    out_ref[...] = (attended * lax.rsqrt(mean_square + EPSILON) * gain_ref[...]).astype(jnp.bfloat16)


def attend(queries, packed, query_at, key_at, value_at, width, lambdas, gains, value_size):
    heads = lambdas.shape[0]
    rows, tokens = queries.shape[0], packed.shape[0]
    query_block = largest_divisor(rows, (512, 384, 256, 128))
    key_block = largest_divisor(tokens, (1024, 1024, 512))
    kernel = functools.partial(
        attention_kernel, score_scale=1.0 / math.sqrt(width // 2), key_block=key_block
    )
    pairs = heads * 2 * rows * tokens
    return pl.pallas_call(
        kernel,
        grid=(heads, rows // query_block),
        in_specs=[
            pl.BlockSpec(memory_space=pltpu.SMEM),
            pl.BlockSpec((query_block, width), lambda h, q: (q, query_at(h))),
            pl.BlockSpec((tokens, width), lambda h, q: (0, key_at(h))),
            pl.BlockSpec((tokens, value_size), lambda h, q: (0, value_at(h))),
            pl.BlockSpec((None, 1, value_size), lambda h, q: (h, 0, 0)),
        ],
        out_specs=pl.BlockSpec((None, query_block, value_size), lambda h, q: (h, q, 0)),
        out_shape=jax.ShapeDtypeStruct((heads, rows, value_size), jnp.bfloat16),
        scratch_shapes=[pltpu.VMEM((tokens, 2 * value_size), jnp.bfloat16)],
        compiler_params=pltpu.CompilerParams(
            dimension_semantics=("arbitrary", "arbitrary"), vmem_limit_bytes=60 * 1024 * 1024
        ),
        cost_estimate=pl.CostEstimate(
            flops=pairs * 1024, bytes_accessed=tokens * (width + value_size) * 2, transcendentals=pairs
        ),
    )(lambdas, queries, packed, packed, gains.reshape(heads, 1, value_size))


class Ring:
    def __init__(self, block, axis, n_sp, forward_hops):
        ring = list(range(0, n_sp, 2)) + list(range(1, n_sp, 2))[::-1]
        position = [0] * n_sp
        for index, member in enumerate(ring):
            position[member] = index
        self.here = jnp.asarray(position, jnp.int32)[lax.axis_index("sp")]
        self.owners = jnp.asarray(ring, jnp.int32)
        self.axis, self.n_sp, self.size = axis, n_sp, block.shape[axis]
        self.forward = [(ring[i], ring[(i + 1) % n_sp]) for i in range(n_sp)]
        self.backward = [(b, a) for a, b in self.forward]
        self.limits = (forward_hops, n_sp - 1 - forward_hops)
        self.ahead, self.behind = block, block
        self.pieces = [(block, 0)]
        self.done = 0

    def hop(self):
        self.done += 1
        if self.done <= self.limits[0]:
            self.ahead = lax.ppermute(self.ahead, "sp", self.forward)
            self.pieces.append((self.ahead, -self.done))
        if self.done <= self.limits[1]:
            self.behind = lax.ppermute(self.behind, "sp", self.backward)
            self.pieces.append((self.behind, self.done))

    def finish(self):
        while self.done < max(self.limits):
            self.hop()
        shape = list(self.pieces[0][0].shape)
        shape[self.axis] = self.size * self.n_sp
        whole = jnp.zeros(tuple(shape), self.ahead.dtype)
        for piece, offset in self.pieces:
            owner = self.owners[lax.rem(self.here + offset + self.n_sp, self.n_sp)]
            whole = lax.dynamic_update_slice_in_dim(whole, piece, owner * self.size, self.axis)
        return whole


def tie(array, rings):
    held = [(ring.ahead, ring.behind) for ring in rings]
    array, held = lax.optimization_barrier((array, held))
    for ring, (ahead, behind) in zip(rings, held):
        ring.ahead, ring.behind = ahead, behind
    return array


def spread(block, n_sp, stride):
    count = n_sp // stride
    forward = [(i, (i + stride) % n_sp) for i in range(n_sp)]
    backward = [(b, a) for a, b in forward]
    pieces = [block]
    ahead, behind = block, block
    for hop in range(1, (count - 1) // 2 + 1):
        ahead = lax.ppermute(ahead, "sp", forward)
        behind = lax.ppermute(behind, "sp", backward)
        pieces += [ahead, behind]
    last = (ahead, behind)
    if count % 2 == 0:
        half = block.shape[0] // 2
        pieces.append(lax.ppermute(ahead[:half], "sp", forward))
        pieces.append(lax.ppermute(behind[half:], "sp", backward))
    return pieces, last


def squared_relu(expanded):
    return jnp.square(jnp.maximum(expanded, 0.0)).astype(jnp.bfloat16)


def local(
    query_first,
    key_first,
    value_first,
    query_second,
    key_second,
    value_second,
    mix_lambda,
    head_gain,
    out_weight,
    residual,
    norm_gain,
    up_weight,
    down_weight,
    n_sp,
):
    tok_dev, local_heads, width_first = query_first.shape
    width_second = query_second.shape[2]
    value_size = value_first.shape[2]
    shares = 2 if local_heads % 2 == 0 and n_sp % 2 == 0 else 1
    heads = local_heads // shares
    place = lax.rem(lax.axis_index("sp"), shares)
    swap = [(i, i ^ 1) for i in range(n_sp)]

    def pick(array, axis, share):
        return lax.dynamic_slice_in_dim(array, share * heads, heads, axis)

    def flat(members, share):
        return jnp.concatenate(
            [pick(member, 1, share).reshape(tok_dev, -1) for member in members], axis=1
        )

    sources = (key_second, key_first, value_first, value_second)
    asked = (query_second, query_first)
    if shares == 2:
        other = lax.ppermute(flat(sources, 1 - place), "sp", swap)
        theirs = lax.ppermute(flat(asked, 1 - place), "sp", swap)
        pieces, unused = spread(flat(sources, place), n_sp, shares)
        more, last = spread(other, n_sp, shares)
        pieces = pieces + more
        queries = jnp.concatenate([flat(asked, place), theirs], axis=0)
    else:
        pieces, last = spread(flat(sources, 0), n_sp, shares)
        queries = flat(asked, 0)
    packed = jnp.concatenate(pieces, axis=0)
    up_weight, down_weight, unused = lax.optimization_barrier((up_weight, down_weight, last))
    rings = (
        Ring(up_weight, 0, n_sp, n_sp // 2),
        Ring(down_weight, 1, n_sp, (n_sp - 1) // 2),
    )
    for ring in rings:
        ring.hop()
    queries = tie(queries, rings)

    lambdas, gains = pick(mix_lambda, 1, place), pick(head_gain, 1, place)
    first_at = heads * width_second // width_first
    value_at = heads * (width_second + width_first) // value_size
    heads_second = attend(
        queries, packed, lambda h: h, lambda h: h, lambda h: value_at + heads + h,
        width_second, lambdas[1], gains[1], value_size,
    )
    for ring in rings:
        ring.hop()
    queries = tie(queries, rings)
    heads_first = attend(
        queries, packed, lambda h: first_at + h, lambda h: first_at + h, lambda h: value_at + h,
        width_first, lambdas[0], gains[0], value_size,
    )
    for ring in rings:
        ring.hop()
    heads_first = tie(heads_first, rings)
    up_whole, down_whole = (ring.finish() for ring in rings)
    mine = jnp.stack([heads_first, heads_second])
    if shares == 2:
        theirs = lax.ppermute(mine[:, :, tok_dev:], "sp", swap)
        mine = mine[:, :, :tok_dev]
        stacked = jnp.where(
            place == 0,
            jnp.concatenate([mine, theirs], axis=1),
            jnp.concatenate([theirs, mine], axis=1),
        )
    else:
        stacked = mine
    projected = lax.psum_scatter(
        jnp.einsum(
            "ghqv,ghvd->qd", stacked, out_weight, preferred_element_type=jnp.float32
        ).astype(jnp.bfloat16),
        "tp",
        scatter_dimension=0,
        tiled=True,
    ).astype(jnp.float32) + residual.astype(jnp.float32)
    normed = layer_norm(projected, norm_gain[0])
    mixer_in = lax.all_gather(normed.astype(jnp.bfloat16), "tp", axis=0, tiled=True)
    hidden = squared_relu(jnp.dot(mixer_in, up_whole, preferred_element_type=jnp.float32))
    mixed_sum = lax.psum_scatter(
        jnp.dot(hidden, down_whole, preferred_element_type=jnp.float32).astype(jnp.bfloat16),
        "tp",
        scatter_dimension=0,
        tiled=True,
    ).astype(jnp.float32)
    return layer_norm(normed + mixed_sum, norm_gain[1]).astype(jnp.bfloat16)


def solution(mesh):
    return jax.shard_map(
        functools.partial(local, n_sp=mesh.shape["sp"]),
        mesh=mesh,
        in_specs=(
            P("sp", "tp", None),
            P("sp", "tp", None),
            P("sp", "tp", None),
            P("sp", "tp", None),
            P("sp", "tp", None),
            P("sp", "tp", None),
            P(None, "tp"),
            P(None, "tp", None),
            P(None, "tp", None, None),
            P(("sp", "tp"), None),
            P(),
            P("sp", "tp"),
            P("tp", "sp"),
        ),
        out_specs=P(("sp", "tp"), None),
        check_vma=False,
    )
```
